32 devices in a mesh: sp: 8 (over z, y), tp: 4 (over x, core).
Axes of the slice: x: 2, y: 2, z: 4, core: 2. Of those that a mesh axis runs over, the one named last changes fastest.
Arguments:
- tokens: bfloat16 [4, 3072, 2048], P(None, 'sp'), may hold values from -21 to 21
- query_weight: bfloat16 [2048, 1024], P(None, 'tp'), may hold values from -0.125 to 0.125
- key_weight: bfloat16 [2048, 1024], P(None, 'tp'), may hold values from -0.125 to 0.125
- value_weight: bfloat16 [2048, 1024], P(None, 'tp'), may hold values from -0.125 to 0.125
- out_gain: float32 [1024], replicated, may hold values from 0.1 to 1.9
- out_weight: bfloat16 [1024, 2048], P(None, 'tp'), may hold values from -0.1875 to 0.1875
Outputs:
- mixed_out: bfloat16 [4, 3072, 2048], P(None, 'sp', 'tp')
- total_log: float32 [4, 8, 3072], P(None, 'tp', 'sp')
The draws below stay inside these ranges and needn't reach their ends.
All inputs are finite; a program needn't handle non-finite values.
Results may differ from the reference program's by a relative error of at most 0.0098.
Values may be sent and summed in bfloat16 or wider, within the bound.
A program may use at most 128 MiB of HBM per device.

```python
import jax
import jax.numpy as jnp
from jax import lax

D = 2048
HEADS = 8
HEAD_DIM = 128
REACH = 64
SEQS = 4
TOK_DEV = 384
TOKENS = 3072


def draw_tokens(key, part):
    dims = (SEQS, TOKENS, D)
    return jnp.clip(jax.random.normal(key, dims, jnp.float32), -6.0, 6.0).astype(jnp.bfloat16)


def block_levels(rng, shape, cuts, least, high):
    factor_of, own = 1.0, jax.random.fold_in(rng, 6)
    for axis_at, blocks in cuts:
        heights = jnp.exp(jax.random.uniform(jax.random.fold_in(own, axis_at), (blocks,), jnp.float32, least / len(cuts), high / len(cuts)))
        factor_of = factor_of * jnp.repeat(heights, shape[axis_at] // blocks).reshape([-1 if axis == axis_at else 1 for axis in range(len(shape))])
    return factor_of


def bell_draw(rng, shape, deviation, bound, cuts=(), kind=jnp.bfloat16):
    entries = jax.random.normal(rng, shape, jnp.float32) * deviation
    if len(cuts) > 0:
        entries = block_levels(rng, shape, cuts, -0.22, 0.18) * entries
    return jnp.clip(entries, min=-bound, max=bound).astype(kind)


def setup_inputs(seed: int = 0) -> dict:
    arg_keys = jax.random.split(jax.random.key(seed), 7)
    tokens = draw_tokens(jax.random.fold_in(arg_keys[6], 71), 0)
    query_weight = bell_draw(arg_keys[1], (D, HEADS * HEAD_DIM), D ** -0.5, 0.125, ((1, 4),))
    key_weight = bell_draw(arg_keys[2], (D, HEADS * HEAD_DIM), D ** -0.5, 0.125, ((1, 4),))
    value_weight = bell_draw(arg_keys[3], (D, HEADS * HEAD_DIM), D ** -0.5, 0.125, ((1, 4),))
    out_gain = jnp.clip(1.0 + 0.18 * jax.random.normal(arg_keys[4], (HEADS * HEAD_DIM,), jnp.float32), 0.1, 1.9)
    out_weight = bell_draw(arg_keys[5], (HEADS * HEAD_DIM, D), (HEADS * HEAD_DIM) ** -0.5, 0.1875, ((1, 4),))
    return {"tokens": tokens, "query_weight": query_weight, "key_weight": key_weight, "value_weight": value_weight, "out_gain": out_gain, "out_weight": out_weight}


DILATIONS = (1, 4, 16)
ROPE_BASE = 10000.0
MASK_FILL = -1e+30
NORM_FLOOR = 1e-06

def rotate(projected, positions):
    in_shape = projected.shape
    heads_view = projected.reshape(in_shape[0], in_shape[1], -1, HEAD_DIM)
    half_dim = HEAD_DIM // 2
    frequency = ROPE_BASE ** (-jnp.arange(half_dim, dtype=jnp.float32) / half_dim)
    angles = positions.astype(jnp.float32)[:, None] * frequency[None, :]
    cosine = jnp.cos(angles)[None, :, None, :]
    sine_part = jnp.sin(angles)[None, :, None, :]
    lower_half = heads_view[..., :half_dim]
    upper_half = heads_view[..., half_dim:]
    turned = jnp.concatenate([lower_half * cosine - upper_half * sine_part, upper_half * cosine + lower_half * sine_part], axis=-1)
    return turned.reshape(in_shape)

def band_attend(queries, extended, dilation, offset, total_len):
    seq_count, length, channels = queries.shape
    head_count = channels // HEAD_DIM
    reach_span = REACH * dilation
    query_rows = length // dilation
    key_rows = query_rows + 2 * REACH
    shaped_q = queries.reshape(seq_count, query_rows, dilation, head_count, HEAD_DIM).astype(jnp.float32)
    shaped_k = extended[:, :, :channels].reshape(seq_count, key_rows, dilation, head_count, HEAD_DIM).astype(jnp.float32)
    shaped_v = extended[:, :, channels:].reshape(seq_count, key_rows, dilation, head_count, HEAD_DIM).astype(jnp.float32)
    scores = jnp.einsum('sarhe,sbrhe->srhab', shaped_q, shaped_k)
    query_row = jnp.arange(query_rows, dtype=jnp.int32)[:, None]
    key_row = jnp.arange(key_rows, dtype=jnp.int32)[None, :]
    inband = (key_row >= query_row) & (key_row <= query_row + 2 * REACH)
    residue = jnp.arange(dilation, dtype=jnp.int32)[:, None, None]
    key_pos = offset - reach_span + key_row[None] * dilation + residue
    allowed = inband[None] & (key_pos >= 0) & (key_pos < total_len)
    scores = jnp.where(allowed[None, :, None], scores * HEAD_DIM ** (-0.5), MASK_FILL)
    maximum = lax.optimization_barrier(jnp.max(scores, axis=-1, keepdims=True))
    exp_scores = jnp.exp(scores - maximum)
    weight_sum = lax.optimization_barrier(jnp.sum(exp_scores, axis=-1, keepdims=True))
    probs = lax.optimization_barrier(exp_scores.astype(jnp.bfloat16)).astype(jnp.float32)
    branch = jnp.einsum('srhab,sbrhe->sarhe', probs, shaped_v)
    branch = branch / jnp.transpose(weight_sum, (0, 3, 1, 2, 4))
    branch = branch.reshape(seq_count, length, head_count, HEAD_DIM)
    log_sum = (maximum + jnp.log(weight_sum))[..., 0]
    log_sum = jnp.transpose(log_sum, (0, 2, 3, 1)).reshape(seq_count, head_count, length)
    return (branch, log_sum)

def combine(branch_out, branch_log):
    logs = jnp.stack(branch_log, 0)
    peak = lax.optimization_barrier(jnp.max(logs, axis=0))
    total_log = peak + jnp.log(lax.optimization_barrier(jnp.sum(jnp.exp(logs - peak[None]), axis=0)))
    shares = jnp.exp(logs - total_log[None])
    shares = jnp.transpose(shares, (0, 1, 3, 2))[..., None]
    merged = lax.optimization_barrier(jnp.sum(shares * jnp.stack(branch_out, 0), axis=0))
    seq_count, length, head_count, head_dim = merged.shape
    return (merged.reshape(seq_count, length, head_count * head_dim).astype(jnp.bfloat16), total_log)

def reference(tokens, query_weight, key_weight, value_weight, out_gain, out_weight):
    flat_rows = tokens.reshape(SEQS * TOKENS, D)
    positions = jnp.arange(TOKENS, dtype=jnp.int32)

    def project(weight):
        return jnp.dot(flat_rows, weight, preferred_element_type=jnp.float32).reshape(SEQS, TOKENS, -1)
    queries = rotate(project(query_weight), positions).astype(jnp.bfloat16)
    key_rows = rotate(project(key_weight), positions).astype(jnp.bfloat16)
    values = project(value_weight).astype(jnp.bfloat16)
    wide_span = REACH * DILATIONS[2]
    stacked = jnp.pad(jnp.concatenate([key_rows, values], axis=2), ((0, 0), (wide_span, wide_span), (0, 0)))

    def one_block(block_index):
        row_start = (block_index * TOK_DEV).astype(jnp.int32)
        block_q = lax.dynamic_slice_in_dim(queries, row_start, TOK_DEV, 1)
        branch_out = []
        branch_log = []
        for dilation in DILATIONS:
            reach_span = REACH * dilation
            extended = lax.dynamic_slice_in_dim(stacked, row_start + wide_span - reach_span, TOK_DEV + 2 * reach_span, 1)
            branch, log_sum = band_attend(block_q, extended, dilation, row_start, TOKENS)
            branch_out.append(branch)
            branch_log.append(log_sum)
        return combine(branch_out, branch_log)
    merged, total_log = lax.map(one_block, jnp.arange(TOKENS // TOK_DEV, dtype=jnp.int32))
    merged = jnp.transpose(merged, (1, 0, 2, 3)).reshape(SEQS, TOKENS, HEADS * HEAD_DIM)
    total_log = jnp.transpose(total_log, (1, 2, 0, 3)).reshape(SEQS, HEADS, TOKENS)
    lifted = merged.astype(jnp.float32)
    square = lax.optimization_barrier(jnp.mean(lifted * lifted, axis=-1))
    scaled = (lifted * out_gain.astype(jnp.float32)).astype(jnp.bfloat16)
    projected = jnp.dot(scaled.reshape(SEQS * TOKENS, HEADS * HEAD_DIM), out_weight, preferred_element_type=jnp.float32).reshape(SEQS, TOKENS, D)
    mixed_out = (projected * lax.rsqrt(square + NORM_FLOOR)[..., None]).astype(jnp.bfloat16)
    return (mixed_out, total_log)
```

```python
import functools
import math

import jax
import jax.numpy as jnp
from jax import lax
from jax.experimental import pallas as pl
from jax.experimental.pallas import tpu as pltpu
from jax.sharding import PartitionSpec as P

HEAD_DIM = 128
REACH = 64
FAR = 16
NEAR = 4
GRAN = FAR * FAR
ROPE_BASE = 10000.0
MASK_FILL = -1e30
NORM_FLOOR = 1e-06
LOG2E = 1.0 / math.log(2.0)
LN2 = math.log(2.0)
F32 = jnp.float32
BF16 = jnp.bfloat16


def shift(block, axis, distance):
    size = lax.axis_size(axis)
    route = [(i - distance, i) for i in range(size) if 0 <= i - distance < size]
    return lax.ppermute(block, axis, route)


def swap(block, axis, bit):
    size = lax.axis_size(axis)
    return lax.ppermute(block, axis, [(i, i ^ bit) for i in range(size)])


def project_kernel(info, tok, wq, wk, wv, cos, sin, q_out, kv_out):
    x = tok[0]
    c, s = cos[...], sin[...]

    def turned(w):
        a = jnp.dot(x, w[...], preferred_element_type=F32)
        parts = []
        for h in range(a.shape[1] // HEAD_DIM):
            one = a[:, h * HEAD_DIM : (h + 1) * HEAD_DIM]
            parts.append((one * c + pltpu.roll(one, HEAD_DIM // 2, 1) * s).astype(BF16))
        return parts

    for h, part in enumerate(turned(wq)):
        q_out[0, :, h * HEAD_DIM : (h + 1) * HEAD_DIM] = part
    for h, part in enumerate(turned(wk)):
        kv_out[0, :, 2 * h * HEAD_DIM : (2 * h + 1) * HEAD_DIM] = part
    v = jnp.dot(x, wv[...], preferred_element_type=F32).astype(BF16)
    for h in range(v.shape[1] // HEAD_DIM):
        kv_out[0, :, (2 * h + 1) * HEAD_DIM : (2 * h + 2) * HEAD_DIM] = v[
            :, h * HEAD_DIM : (h + 1) * HEAD_DIM
        ]


def project(info, tokens, wq, wk, wv, cos, sin, mine):
    seqs, length, width = tokens.shape
    half = seqs // 2
    cols = wq.shape[1]

    def tok_map(i, info):
        group = info[0] if mine else 1 - info[0]
        return (group * half + i, 0, 0)

    whole = lambda i, info: (0, 0)
    return pl.pallas_call(
        project_kernel,
        grid_spec=pltpu.PrefetchScalarGridSpec(
            num_scalar_prefetch=1,
            grid=(half,),
            in_specs=[
                pl.BlockSpec((1, length, width), tok_map),
                pl.BlockSpec((width, cols), whole),
                pl.BlockSpec((width, cols), whole),
                pl.BlockSpec((width, cols), whole),
                pl.BlockSpec((length, HEAD_DIM), whole),
                pl.BlockSpec((length, HEAD_DIM), whole),
            ],
            out_specs=[
                pl.BlockSpec((1, length, cols), lambda i, info: (i, 0, 0)),
                pl.BlockSpec((1, length, 2 * cols), lambda i, info: (i, 0, 0)),
            ],
        ),
        out_shape=[
            jax.ShapeDtypeStruct((half, length, cols), BF16),
            jax.ShapeDtypeStruct((half, length, 2 * cols), BF16),
        ],
        compiler_params=pltpu.CompilerParams(
            dimension_semantics=("arbitrary",), vmem_limit_bytes=40 * 2**20
        ),
        cost_estimate=pl.CostEstimate(
            flops=2 * half * length * width * 3 * cols,
            bytes_accessed=2 * (half * length * width + 3 * width * cols),
            transcendentals=0,
        ),
        name="project",
    )(info, tokens, wq, wk, wv, cos, sin)


def iota(shape, dim):
    return lax.broadcasted_iota(jnp.int32, shape, dim)


def perm_token(p):
    slot = p // FAR
    a = p % FAR
    residue = slot // NEAR + NEAR * (slot % (FAR // NEAR))
    return a * FAR + residue


def dot_t(a, b):
    return lax.dot_general(a, b, (((1,), (1,)), ((), ())), preferred_element_type=F32)


def attend_kernel(
    total, info, fl, la, lb, oa, ob, ra, rb, fr, qa, qb, out_m, out_o, log_out,
    kn, kp, qp, mp, on, perm, bias1, bias4, bias16, o1, m1, l1,
):
    length = oa.shape[1]
    block = 2 * length
    wide = REACH * FAR
    grans = block // GRAN
    side = wide // GRAN
    tail = fl.shape[1]
    span = block + 2 * wide
    rows = block // FAR
    key_rows = span // FAR
    near_rows = rows + 2 * FAR
    y, blk = info[0], info[1]
    scale = HEAD_DIM**-0.5 * LOG2E

    @pl.when((pl.program_id(0) == 0) & (pl.program_id(1) == 0))
    def _():
        perm[...] = jnp.where(
            iota((GRAN, GRAN), 1) == perm_token(iota((GRAN, GRAN), 0)), 1.0, 0.0
        ).astype(BF16)
        start = blk * block - wide
        shape = (GRAN, GRAN + 2 * REACH)
        t = perm_token(iota(shape, 0))
        for g in range(grans):
            q_at = wide + g * GRAN + t
            k_at = wide + g * GRAN - REACH + iota(shape, 1)
            ok = (jnp.abs(k_at - q_at) <= REACH) & (k_at + start >= 0) & (k_at + start < total)
            bias1[g] = jnp.where(ok, 0.0, MASK_FILL)
        per = FAR // NEAR
        shape = (per * rows, per * near_rows)
        row, col = iota(shape, 0), iota(shape, 1)
        q_at = (row % rows + side * FAR) * FAR + NEAR * (row // rows)
        k_at = (col % near_rows + (side - 1) * FAR) * FAR + NEAR * (col // near_rows)
        ok = (jnp.abs(k_at - q_at) <= REACH * NEAR) & (k_at + start >= 0) & (k_at + start < total)
        bias4[...] = jnp.where(ok, 0.0, MASK_FILL)
        shape = (rows, key_rows)
        q_at = iota(shape, 0) + side * FAR
        k_at = iota(shape, 1)
        ok = (
            (jnp.abs(k_at - q_at) <= REACH)
            & (k_at * FAR + start >= 0)
            & (k_at * FAR + start < total)
        )
        bias16[...] = jnp.where(ok, 0.0, MASK_FILL)

    first = pl.multiple_of(y * length, HEAD_DIM)
    second = pl.multiple_of((1 - y) * length, HEAD_DIM)
    kn[:tail] = fl[0]
    kn[pl.ds(tail + first, length)] = la[0]
    kn[pl.ds(tail + second, length)] = lb[0]
    kn[pl.ds(wide + first, length)] = oa[0]
    kn[pl.ds(wide + second, length)] = ob[0]
    kn[pl.ds(wide + block + first, length)] = ra[0]
    kn[pl.ds(wide + block + second, length)] = rb[0]
    kn[span - tail :] = fr[0]
    on[pl.ds(first, length)] = qa[0]
    on[pl.ds(second, length)] = qb[0]

    shuffle = perm[...]
    for j in range(span // GRAN):
        moved = jnp.dot(shuffle, kn[j * GRAN : (j + 1) * GRAN], preferred_element_type=F32)
        kp[:, j * FAR : (j + 1) * FAR] = moved.astype(BF16).reshape(FAR, FAR, 2 * HEAD_DIM)
    for g in range(grans):
        moved = jnp.dot(shuffle, on[g * GRAN : (g + 1) * GRAN], preferred_element_type=F32)
        moved = moved.astype(BF16)
        qp[:, g * FAR : (g + 1) * FAR] = moved.reshape(FAR, FAR, HEAD_DIM)
        at = wide + g * GRAN - REACH
        k = kn[at : at + GRAN + 2 * REACH, :HEAD_DIM]
        v = kn[at : at + GRAN + 2 * REACH, HEAD_DIM:]
        s = dot_t(moved, k) * scale + bias1[g]
        m = jnp.max(s, axis=1, keepdims=True)
        p = jnp.exp2(s - m)
        l = jnp.sum(p, axis=1, keepdims=True)
        o = jnp.dot(p.astype(BF16), v, preferred_element_type=F32)
        cut = (FAR, FAR, HEAD_DIM)
        o1[:, g * FAR : (g + 1) * FAR] = o.reshape(cut)
        m1[:, g * FAR : (g + 1) * FAR] = jnp.broadcast_to(m, o.shape).reshape(cut)
        l1[:, g * FAR : (g + 1) * FAR] = jnp.broadcast_to(l, o.shape).reshape(cut)

    per = FAR // NEAR
    near_at = (side - 1) * FAR
    for group in range(NEAR):
        sel = slice(group * per, (group + 1) * per)
        flat = (per * rows, HEAD_DIM)
        q = qp[sel].reshape(flat)
        k4 = kp[sel, near_at : near_at + near_rows, :HEAD_DIM].reshape(-1, HEAD_DIM)
        v4 = kp[sel, near_at : near_at + near_rows, HEAD_DIM:].reshape(-1, HEAD_DIM)
        s4 = dot_t(q, k4) * scale + bias4[...]
        b16 = bias16[...]
        s16 = jnp.concatenate(
            [
                dot_t(qp[group * per + i], kp[group * per + i, :, :HEAD_DIM]) * scale + b16
                for i in range(per)
            ],
            axis=0,
        )
        m_old = m1[sel].reshape(flat)
        m_row = jnp.maximum(
            jnp.max(s4, axis=1, keepdims=True), jnp.max(s16, axis=1, keepdims=True)
        )
        m_new = jnp.maximum(m_old, m_row)
        m_col = m_new[:, :1]
        keep = jnp.exp2(m_old - m_new)
        p4 = jnp.exp2(s4 - m_col)
        p16 = jnp.exp2(s16 - m_col)
        l = l1[sel].reshape(flat) * keep + (
            jnp.sum(p4, axis=1, keepdims=True) + jnp.sum(p16, axis=1, keepdims=True)
        )
        p16 = p16.astype(BF16)
        o16 = jnp.concatenate(
            [
                jnp.dot(
                    p16[i * rows : (i + 1) * rows],
                    kp[group * per + i, :, HEAD_DIM:],
                    preferred_element_type=F32,
                )
                for i in range(per)
            ],
            axis=0,
        )
        o = o1[sel].reshape(flat) * keep + o16
        o = o + jnp.dot(p4.astype(BF16), v4, preferred_element_type=F32)
        mp[sel] = (o / l).astype(BF16).reshape(per, rows, HEAD_DIM)
        m1[sel] = (m_new * LN2 + jnp.log(l)).reshape(per, rows, HEAD_DIM)

    lane = iota((GRAN, HEAD_DIM), 1)
    for g in range(grans):
        cut = slice(g * FAR, (g + 1) * FAR)
        back = lambda a: lax.dot_general(
            a, shuffle, (((0,), (0,)), ((), ())), preferred_element_type=F32
        )
        merged = lax.dot_general(
            shuffle,
            mp[:, cut].reshape(GRAN, HEAD_DIM),
            (((0,), (0,)), ((), ())),
            preferred_element_type=F32,
        )
        on[g * GRAN : (g + 1) * GRAN] = merged.astype(BF16)
        x = m1[:, cut].reshape(GRAN, HEAD_DIM)
        high = x.astype(BF16).astype(F32)
        mid = (x - high).astype(BF16).astype(F32)
        low = x - high - mid
        terms = jnp.where(lane == 0, high, jnp.where(lane == 1, mid, jnp.where(lane == 2, low, 0.0)))
        log_out[0, 0, :, g * GRAN : (g + 1) * GRAN] = jnp.sum(
            back(terms.astype(BF16)), axis=0, keepdims=True
        )
    out_m[0] = on[pl.ds(first, length)]
    out_o[0] = on[pl.ds(second, length)]


def attend(info, total, fl, la, lb, oa, ob, ra, rb, fr, qa, qb):
    seqs, length, channels = qa.shape
    heads = channels // HEAD_DIM
    block = 2 * length
    wide = REACH * FAR
    span = block + 2 * wide
    rows = block // FAR
    near_rows = rows + 2 * FAR
    per = FAR // NEAR
    grans = block // GRAN
    at = lambda s, h, info: (s, 0, h)
    kv_spec = lambda n: pl.BlockSpec((1, n, 2 * HEAD_DIM), at)
    q_spec = pl.BlockSpec((1, length, HEAD_DIM), at)
    return pl.pallas_call(
        functools.partial(attend_kernel, total),
        grid_spec=pltpu.PrefetchScalarGridSpec(
            num_scalar_prefetch=1,
            grid=(seqs, heads),
            in_specs=[kv_spec(a.shape[1]) for a in (fl, la, lb, oa, ob, ra, rb, fr)]
            + [q_spec, q_spec],
            out_specs=[
                q_spec,
                q_spec,
                pl.BlockSpec((1, 1, 1, block), lambda s, h, info: (s, h, 0, 0)),
            ],
            scratch_shapes=[
                pltpu.VMEM((span, 2 * HEAD_DIM), BF16),
                pltpu.VMEM((FAR, span // FAR, 2 * HEAD_DIM), BF16),
                pltpu.VMEM((FAR, rows, HEAD_DIM), BF16),
                pltpu.VMEM((FAR, rows, HEAD_DIM), BF16),
                pltpu.VMEM((block, HEAD_DIM), BF16),
                pltpu.VMEM((GRAN, GRAN), BF16),
                pltpu.VMEM((grans, GRAN, GRAN + 2 * REACH), F32),
                pltpu.VMEM((per * rows, per * near_rows), F32),
                pltpu.VMEM((rows, span // FAR), F32),
                pltpu.VMEM((FAR, rows, HEAD_DIM), F32),
                pltpu.VMEM((FAR, rows, HEAD_DIM), F32),
                pltpu.VMEM((FAR, rows, HEAD_DIM), F32),
            ],
        ),
        out_shape=[
            jax.ShapeDtypeStruct((seqs, length, channels), BF16),
            jax.ShapeDtypeStruct((seqs, length, channels), BF16),
            jax.ShapeDtypeStruct((seqs, heads, 1, block), F32),
        ],
        compiler_params=pltpu.CompilerParams(
            dimension_semantics=("arbitrary", "arbitrary"), vmem_limit_bytes=40 * 2**20
        ),
        cost_estimate=pl.CostEstimate(
            flops=seqs * heads * 2**29,
            bytes_accessed=seqs * heads * span * 1024,
            transcendentals=seqs * heads * 2**19,
        ),
        name="attend",
    )(info, fl, la, lb, oa, ob, ra, rb, fr, qa, qb)


def out_kernel(info, *refs):
    m_refs, r_refs, gain, w, out = refs[:4], refs[4:8], refs[8], refs[9], refs[10]
    y, t = info[0], info[2]
    j = pl.program_id(0)
    half = m_refs[0].shape[0]
    cols = m_refs[0].shape[2]

    def run(group):
        total = None
        square = None
        for piece, bit in zip(group, (0, 1, 2, 3)):
            x = piece[j % half].astype(F32)
            at = pl.multiple_of((t ^ bit) * cols, HEAD_DIM)
            scaled = (x * gain[:, pl.ds(at, cols)]).astype(BF16)
            term = jnp.dot(scaled, w[pl.ds(at, cols)], preferred_element_type=F32)
            sq = jnp.sum(x * x, axis=1, keepdims=True)
            total = term if total is None else total + term
            square = sq if square is None else square + sq
        out[0] = (total * lax.rsqrt(square / w.shape[0] + NORM_FLOOR)).astype(BF16)

    @pl.when(j // half == y)
    def _():
        run(m_refs)

    @pl.when(j // half != y)
    def _():
        run(r_refs)


def out_project(info, m_parts, r_parts, gain, w):
    half, length, cols = m_parts[0].shape
    whole3 = pl.BlockSpec((half, length, cols), lambda j, info: (0, 0, 0))
    return pl.pallas_call(
        out_kernel,
        grid_spec=pltpu.PrefetchScalarGridSpec(
            num_scalar_prefetch=1,
            grid=(2 * half,),
            in_specs=[whole3] * 8
            + [
                pl.BlockSpec((1, w.shape[0]), lambda j, info: (0, 0)),
                pl.BlockSpec(w.shape, lambda j, info: (0, 0)),
            ],
            out_specs=pl.BlockSpec((1, length, w.shape[1]), lambda j, info: (j, 0, 0)),
        ),
        out_shape=jax.ShapeDtypeStruct((2 * half, length, w.shape[1]), BF16),
        compiler_params=pltpu.CompilerParams(
            dimension_semantics=("arbitrary",), vmem_limit_bytes=40 * 2**20
        ),
        name="out_project",
    )(info, *m_parts, *r_parts, gain, w)


def shards(tokens, query_weight, key_weight, value_weight, out_gain, out_weight):
    seqs, length, _ = tokens.shape
    sp = lax.axis_index("sp")
    y, blk, t = sp % 2, sp // 2, lax.axis_index("tp")
    info = jnp.stack([y, blk, t]).astype(jnp.int32)
    total = length * lax.axis_size("sp")
    half_dim = HEAD_DIM // 2
    frequency = ROPE_BASE ** (-jnp.arange(half_dim, dtype=F32) / half_dim)
    positions = sp * length + jnp.arange(length, dtype=jnp.int32)
    angles = positions.astype(F32)[:, None] * frequency[None, :]
    cos, sin = jnp.cos(angles), jnp.sin(angles)
    cos = jnp.concatenate([cos, cos], axis=1)
    sin = jnp.concatenate([-sin, sin], axis=1)

    weights = (query_weight, key_weight, value_weight)
    q_o, kv_o = project(info, tokens, *weights, cos, sin, mine=False)
    q_m, kv_m = project(info, tokens, *weights, cos, sin, mine=True)
    kv_r = swap(kv_o, "sp", 1)
    q_r = swap(q_o, "sp", 1)
    la, ra = shift(kv_m, "sp", 2), shift(kv_m, "sp", -2)
    tail = REACH * FAR - 2 * length
    last = jnp.where(y == 1, kv_m[:, length - tail :], kv_r[:, length - tail :])
    head = jnp.where(y == 0, kv_m[:, :tail], kv_r[:, :tail])
    lb, rb = shift(kv_r, "sp", 2), shift(kv_r, "sp", -2)
    fl, fr = shift(last, "sp", 4), shift(head, "sp", -4)

    out_m, out_o, log = attend(info, total, fl, la, lb, kv_m, kv_r, ra, rb, fr, q_m, q_r)
    out_r = swap(out_o, "sp", 1)
    log = log[:, :, 0].reshape(seqs // 2, -1, 2, length)
    log_m = lax.dynamic_index_in_dim(log, y, 2, keepdims=False)
    log_r = swap(lax.dynamic_index_in_dim(log, 1 - y, 2, keepdims=False), "sp", 1)
    total_log = jnp.where(
        y == 0, jnp.concatenate([log_m, log_r], 0), jnp.concatenate([log_r, log_m], 0)
    )
    m2, r2 = swap(out_m, "tp", 2), swap(out_r, "tp", 2)
    m1, r1 = swap(out_m, "tp", 1), swap(out_r, "tp", 1)
    m3, r3 = swap(m2, "tp", 1), swap(r2, "tp", 1)
    mixed = out_project(
        info, (out_m, m1, m2, m3), (out_r, r1, r2, r3), out_gain[None, :], out_weight
    )
    return (mixed, total_log)


def solution(mesh):
    return jax.shard_map(
        shards,
        mesh=mesh,
        in_specs=(
            P(None, "sp", None),
            P(None, "tp"),
            P(None, "tp"),
            P(None, "tp"),
            P(),
            P(None, "tp"),
        ),
        out_specs=(P(None, "sp", "tp"), P(None, "tp", "sp")),
        check_vma=False,
    )
```

```python
import functools
import math

import jax
import jax.numpy as jnp
from jax import lax
from jax.experimental import pallas as pl
from jax.experimental.pallas import tpu as pltpu
from jax.sharding import PartitionSpec as P

HEAD_DIM = 128
REACH = 64
FAR = 16
NEAR = 4
GRAN = FAR * FAR
ROPE_BASE = 10000.0
MASK_FILL = -1e30
NORM_FLOOR = 1e-06
LOG2E = 1.0 / math.log(2.0)
LN2 = math.log(2.0)
F32 = jnp.float32
BF16 = jnp.bfloat16

MESH = pl.DeviceIdType.MESH


def iota(shape, dim):
    return lax.broadcasted_iota(jnp.int32, shape, dim)


def perm_token(p):
    slot = p // FAR
    a = p % FAR
    residue = slot // NEAR + NEAR * (slot % (FAR // NEAR))
    return a * FAR + residue


def dot_t(a, b):
    return lax.dot_general(a, b, (((1,), (1,)), ((), ())), preferred_element_type=F32)


def layer_kernel(
    nsp, tok_h, wq_h, wk_h, wv_h, wo_h, cos_h, sin_h, gain, out, log_out,
    tok, wq, wk, wv, wo, cos, sin, kn, qn, kvs, qs, gath, outs, logs, lsend, lrow,
    kp, qp, mp, on, perm, bias1, bias4, bias16, o1, m1, l1,
    load_sem, send_sem, recv_sem,
):
    half = kn.shape[0]
    length = tok.shape[1]
    block = 2 * length
    grans = block // GRAN
    wide = REACH * FAR
    side = wide // GRAN
    tail = wide - block
    span = block + 2 * wide
    rows = block // FAR
    key_rows = span // FAR
    near_rows = rows + 2 * FAR
    cols = wq.shape[1]
    heads = cols // HEAD_DIM
    total = nsp * length
    scale = HEAD_DIM**-0.5 * LOG2E
    sp, t = lax.axis_index("sp"), lax.axis_index("tp")
    y, blk = sp % 2, sp // 2
    twin = sp + 1 - 2 * y
    x_peer = (t + 2) % 4
    d_peer = t + 1 - 2 * (t % 2)
    x_d_peer = (d_peer + 2) % 4
    mine, other = y * half, (1 - y) * half

    loads = []

    def load(src, dst):
        copy = pltpu.make_async_copy(src, dst, load_sem.at[len(loads)])
        copy.start()
        loads.append(copy)
        return copy

    got_wk, got_wv = load(wk_h, wk), load(wv_h, wv)
    got_tok = {("m", 0): load(tok_h.at[mine], tok.at[0])}
    got_cos, got_sin = load(cos_h, cos), load(sin_h, sin)
    got_tok["o", 0] = load(tok_h.at[other], tok.at[1])
    for s in range(1, half):
        got_tok["o", s] = load(tok_h.at[other + s], tok.at[2 * s + 1])
        got_tok["m", s] = load(tok_h.at[mine + s], tok.at[2 * s])
    got_wq, got_wo = load(wq_h, wq), load(wo_h, wo)

    barrier = pltpu.get_barrier_semaphore()
    has = {d: (sp + d >= 0) & (sp + d < nsp) for d in (2, -2, 4, -4)}
    for peer in ((twin, t), (sp, x_peer), (sp, d_peer)):
        pl.semaphore_signal(barrier, inc=1, device_id=peer, device_id_type=MESH)
    count = 3
    for d, there in has.items():
        count = count + there.astype(jnp.int32)

        @pl.when(there)
        def _(d=d):
            pl.semaphore_signal(barrier, inc=1, device_id=(sp + d, t), device_id_type=MESH)

    first = pl.multiple_of(y * length, HEAD_DIM)
    second = pl.multiple_of((1 - y) * length, HEAD_DIM)

    def clear(d, at, size):
        @pl.when(jnp.logical_not(has[d]))
        def _():
            for s in range(half):
                kn[s, at : at + size] = jnp.zeros((size, kn.shape[2]), BF16)

    clear(-4, 0, tail)
    clear(-2, tail, block)
    clear(2, wide + block, block)
    clear(4, span - tail, tail)

    numbers = {}

    def copy(name, src, dst, peer):
        n = numbers.setdefault(name, len(numbers))
        return pltpu.make_async_remote_copy(
            src_ref=src, dst_ref=dst, send_sem=send_sem.at[n], recv_sem=recv_sem.at[n],
            device_id=peer, device_id_type=MESH,
        )

    sent = []

    def start(c):
        c.start()
        sent.append((c, None))

    def z_copy(kind, s, d):
        peer = (sp + d, t)
        far = kind == "T"
        if far:
            src = wide + (block - tail if d > 0 else 0)
            dst = 0 if d > 0 else span - tail
            size = tail
        else:
            part = first if kind == "A" else second
            src = wide + part
            dst = (tail if d > 0 else wide + block) + part
            size = length
        return copy((kind, s, d), kn.at[s, pl.ds(src, size)], kn.at[s, pl.ds(dst, size)], peer)

    def z_start(kind, s):
        for d in (4, -4) if kind == "T" else (2, -2):
            c = z_copy(kind, s, d)

            @pl.when(has[d])
            def _():
                c.start()

            sent.append((c, has[d]))

    def z_wait(kind, s):
        for d in (4, -4) if kind == "T" else (2, -2):

            @pl.when(has[-d])
            def _():
                z_copy(kind, s, d).wait_recv()

    def turned(x, w, store):
        a = jnp.dot(x, w[...], preferred_element_type=F32)
        for h in range(heads):
            one = a[:, h * HEAD_DIM : (h + 1) * HEAD_DIM]
            store(h, (one * cos[...] + pltpu.roll(one, HEAD_DIM // 2, 1) * sin[...]).astype(BF16))

    def lanes(n):
        return slice(n * HEAD_DIM, (n + 1) * HEAD_DIM)

    def keys_values(x, put):
        turned(x, wk, lambda h, a: put(2 * h, a))
        v = jnp.dot(x, wv[...], preferred_element_type=F32).astype(BF16)
        for h in range(heads):
            put(2 * h + 1, v[:, lanes(h)])

    def own_kv(s):
        def put(n, a):
            kn[s, pl.ds(wide + first, length), lanes(n)] = a

        keys_values(tok[2 * s], put)

    def twin_kv(s):
        def put(n, a):
            kvs[s, :, lanes(n)] = a

        keys_values(tok[2 * s + 1], put)

    def own_q(s):
        def put(n, a):
            qn[s, pl.ds(first, length), lanes(n)] = a

        turned(tok[2 * s], wq, put)

    def twin_q(s):
        def put(n, a):
            qs[s, :, lanes(n)] = a

        turned(tok[2 * s + 1], wq, put)

    def y_kv(s, at):
        return copy(("yk", s), kvs.at[s], kn.at[s, pl.ds(wide + at, length)], (twin, t))

    def y_q(s, at):
        return copy(("yq", s), qs.at[s], qn.at[s, pl.ds(at, length)], (twin, t))

    for c in (got_wk, got_wv, got_cos, got_sin, got_tok["m", 0]):
        c.wait()
    own_kv(0)
    pl.semaphore_wait(barrier, count)
    z_start("A", 0)
    got_tok["o", 0].wait()
    twin_kv(0)
    start(y_kv(0, first))
    for s in range(1, half):
        got_tok["o", s].wait()
        got_tok["m", s].wait()
        twin_kv(s)
        start(y_kv(s, first))
        own_kv(s)
    got_wq.wait()
    for s in range(half):
        twin_q(s)
        own_q(s)
        if s == 0:
            y_kv(0, second).wait_recv()
            z_start("B", 0)
            z_start("T", 0)
        start(y_q(s, first))
    for s in range(1, half):
        z_start("A", s)
        y_kv(s, second).wait_recv()
        z_start("B", s)
        z_start("T", s)

    perm[...] = jnp.where(
        iota((GRAN, GRAN), 1) == perm_token(iota((GRAN, GRAN), 0)), 1.0, 0.0
    ).astype(BF16)
    origin = blk * block - wide
    shape = (GRAN, GRAN + 2 * REACH)
    token = perm_token(iota(shape, 0))
    for g in range(grans):
        q_at = wide + g * GRAN + token
        k_at = wide + g * GRAN - REACH + iota(shape, 1)
        ok = (jnp.abs(k_at - q_at) <= REACH) & (k_at + origin >= 0) & (k_at + origin < total)
        bias1[g] = jnp.where(ok, 0.0, MASK_FILL)
    per = FAR // NEAR
    shape = (per * rows, per * near_rows)
    row, col = iota(shape, 0), iota(shape, 1)
    q_at = (row % rows + side * FAR) * FAR + NEAR * (row // rows)
    k_at = (col % near_rows + (side - 1) * FAR) * FAR + NEAR * (col // near_rows)
    ok = (jnp.abs(k_at - q_at) <= REACH * NEAR) & (k_at + origin >= 0) & (k_at + origin < total)
    bias4[...] = jnp.where(ok, 0.0, MASK_FILL)
    shape = (rows, key_rows)
    q_at = iota(shape, 0) + side * FAR
    k_at = iota(shape, 1)
    ok = (
        (jnp.abs(k_at - q_at) <= REACH)
        & (k_at * FAR + origin >= 0)
        & (k_at * FAR + origin < total)
    )
    bias16[...] = jnp.where(ok, 0.0, MASK_FILL)

    def attend(s, h):
        kv_lanes = pl.ds(pl.multiple_of(h * 2 * HEAD_DIM, HEAD_DIM), 2 * HEAD_DIM)
        k_lanes = pl.ds(pl.multiple_of(h * 2 * HEAD_DIM, HEAD_DIM), HEAD_DIM)
        v_lanes = pl.ds(pl.multiple_of((h * 2 + 1) * HEAD_DIM, HEAD_DIM), HEAD_DIM)
        h_lanes = pl.ds(pl.multiple_of(h * HEAD_DIM, HEAD_DIM), HEAD_DIM)
        shuffle = perm[...]
        for j in range(span // GRAN):
            moved = jnp.dot(
                shuffle, kn[s, j * GRAN : (j + 1) * GRAN, kv_lanes], preferred_element_type=F32
            )
            kp[:, j * FAR : (j + 1) * FAR] = moved.astype(BF16).reshape(FAR, FAR, 2 * HEAD_DIM)
        for g in range(grans):
            moved = jnp.dot(
                shuffle, qn[s, g * GRAN : (g + 1) * GRAN, h_lanes], preferred_element_type=F32
            )
            moved = moved.astype(BF16)
            qp[:, g * FAR : (g + 1) * FAR] = moved.reshape(FAR, FAR, HEAD_DIM)
            at = wide + g * GRAN - REACH
            k = kn[s, at : at + GRAN + 2 * REACH, k_lanes]
            v = kn[s, at : at + GRAN + 2 * REACH, v_lanes]
            sc = dot_t(moved, k) * scale + bias1[g]
            m = jnp.max(sc, axis=1, keepdims=True)
            p = jnp.exp2(sc - m)
            l = jnp.sum(p, axis=1, keepdims=True)
            o = jnp.dot(p.astype(BF16), v, preferred_element_type=F32)
            cut = (FAR, FAR, HEAD_DIM)
            o1[:, g * FAR : (g + 1) * FAR] = o.reshape(cut)
            m1[:, g * FAR : (g + 1) * FAR] = jnp.broadcast_to(m, o.shape).reshape(cut)
            l1[:, g * FAR : (g + 1) * FAR] = jnp.broadcast_to(l, o.shape).reshape(cut)
        near_at = (side - 1) * FAR
        for group in range(NEAR):
            sel = slice(group * per, (group + 1) * per)
            flat = (per * rows, HEAD_DIM)
            q = qp[sel].reshape(flat)
            k4 = kp[sel, near_at : near_at + near_rows, :HEAD_DIM].reshape(-1, HEAD_DIM)
            v4 = kp[sel, near_at : near_at + near_rows, HEAD_DIM:].reshape(-1, HEAD_DIM)
            s4 = dot_t(q, k4) * scale + bias4[...]
            b16 = bias16[...]
            s16 = jnp.concatenate(
                [
                    dot_t(qp[group * per + i], kp[group * per + i, :, :HEAD_DIM]) * scale + b16
                    for i in range(per)
                ],
                axis=0,
            )
            m_old = m1[sel].reshape(flat)
            m_row = jnp.maximum(
                jnp.max(s4, axis=1, keepdims=True), jnp.max(s16, axis=1, keepdims=True)
            )
            m_new = jnp.maximum(m_old, m_row)
            m_col = m_new[:, :1]
            keep = jnp.exp2(m_old - m_new)
            p4 = jnp.exp2(s4 - m_col)
            p16 = jnp.exp2(s16 - m_col)
            l = l1[sel].reshape(flat) * keep + (
                jnp.sum(p4, axis=1, keepdims=True) + jnp.sum(p16, axis=1, keepdims=True)
            )
            p16 = p16.astype(BF16)
            o16 = jnp.concatenate(
                [
                    jnp.dot(
                        p16[i * rows : (i + 1) * rows],
                        kp[group * per + i, :, HEAD_DIM:],
                        preferred_element_type=F32,
                    )
                    for i in range(per)
                ],
                axis=0,
            )
            o = o1[sel].reshape(flat) * keep + o16
            o = o + jnp.dot(p4.astype(BF16), v4, preferred_element_type=F32)
            mp[sel] = (o / l).astype(BF16).reshape(per, rows, HEAD_DIM)
            m1[sel] = (m_new * LN2 + jnp.log(l)).reshape(per, rows, HEAD_DIM)
        lane = iota((GRAN, HEAD_DIM), 1)
        for g in range(grans):
            cut = slice(g * FAR, (g + 1) * FAR)
            back = lambda a: lax.dot_general(
                a, shuffle, (((0,), (0,)), ((), ())), preferred_element_type=F32
            )
            merged = lax.dot_general(
                shuffle,
                mp[:, cut].reshape(GRAN, HEAD_DIM),
                (((0,), (0,)), ((), ())),
                preferred_element_type=F32,
            )
            on[g * GRAN : (g + 1) * GRAN] = merged.astype(BF16)
            x = m1[:, cut].reshape(GRAN, HEAD_DIM)
            high = x.astype(BF16).astype(F32)
            mid = (x - high).astype(BF16).astype(F32)
            low = x - high - mid
            terms = jnp.where(
                lane == 0, high, jnp.where(lane == 1, mid, jnp.where(lane == 2, low, 0.0))
            )
            lrow[:, g * GRAN : (g + 1) * GRAN] = jnp.sum(
                back(terms.astype(BF16)), axis=0, keepdims=True
            )
        outs[s, :, h_lanes] = on[pl.ds(second, length)]
        gath[t, mine + s, :, h_lanes] = on[pl.ds(first, length)]
        logs[mine + s, pl.ds(h, 1)] = lrow[:, pl.ds(first, length)]
        lsend[s, pl.ds(h, 1)] = lrow[:, pl.ds(second, length)]

    def piece(name, s, owner, j, peer):
        return copy((name, s), gath.at[owner, j], gath.at[owner, j], peer)

    def finish(j):
        acc = None
        square = None
        for n in range(gath.shape[0]):
            x = gath[n, j].astype(F32)
            at = slice(n * cols, (n + 1) * cols)
            scaled = (x * gain[:, at]).astype(BF16)
            term = jnp.dot(scaled, wo[at], preferred_element_type=F32)
            sq = jnp.sum(x * x, axis=1, keepdims=True)
            acc = term if acc is None else acc + term
            square = sq if square is None else square + sq
        out[j] = (acc * lax.rsqrt(square / wo.shape[0] + NORM_FLOOR)).astype(BF16)

    for s in range(half):
        y_q(s, second).wait_recv()
        for kind in ("A", "B", "T"):
            z_wait(kind, s)

        def one(h, carry, s=s):
            attend(s, h)
            return carry

        lax.fori_loop(0, heads, one, 0)
        start(copy(("yo", s), outs.at[s], gath.at[t, mine + s], (twin, t)))
        start(piece("xm", s, t, mine + s, (sp, x_peer)))
        start(copy(("yl", s), lsend.at[s], logs.at[mine + s], (twin, t)))
        start(piece("dm", s, t, mine + s, (sp, d_peer)))
        copy(("yo", s), outs.at[s], gath.at[t, other + s], (twin, t)).wait_recv()
        start(piece("xr", s, t, other + s, (sp, x_peer)))
        start(piece("dr", s, t, other + s, (sp, d_peer)))
        if s == 0:
            got_wo.wait()
        piece("xm", s, x_peer, mine + s, (sp, x_peer)).wait_recv()
        start(piece("em", s, x_peer, mine + s, (sp, d_peer)))
        piece("dm", s, d_peer, mine + s, (sp, d_peer)).wait_recv()
        piece("em", s, x_d_peer, mine + s, (sp, d_peer)).wait_recv()
        finish(mine + s)
        piece("xr", s, x_peer, other + s, (sp, x_peer)).wait_recv()
        start(piece("er", s, x_peer, other + s, (sp, d_peer)))
        piece("dr", s, d_peer, other + s, (sp, d_peer)).wait_recv()
        piece("er", s, x_d_peer, other + s, (sp, d_peer)).wait_recv()
        finish(other + s)
        copy(("yl", s), lsend.at[s], logs.at[other + s], (twin, t)).wait_recv()
    log_out[...] = logs[...]
    for c, there in sent:
        if there is None:
            c.wait_send()
        else:

            @pl.when(there)
            def _(c=c):
                c.wait_send()


def layer(nsp, ntp, tokens, wq, wk, wv, wo, cos, sin, gain):
    seqs, length, width = tokens.shape
    half = seqs // 2
    cols = wq.shape[1]
    heads = cols // HEAD_DIM
    block = 2 * length
    wide = REACH * FAR
    span = block + 2 * wide
    rows = block // FAR
    near_rows = rows + 2 * FAR
    per = FAR // NEAR
    grans = block // GRAN
    hbm = pl.BlockSpec(memory_space=pl.ANY)
    vmem = pl.BlockSpec(memory_space=pltpu.VMEM)
    v = pltpu.VMEM
    return pl.pallas_call(
        functools.partial(layer_kernel, nsp),
        in_specs=[hbm] * 7 + [vmem],
        out_specs=[vmem, vmem],
        out_shape=[
            jax.ShapeDtypeStruct((seqs, length, wo.shape[1]), BF16),
            jax.ShapeDtypeStruct((seqs, heads, length), F32),
        ],
        scratch_shapes=[
            v(tokens.shape, BF16), v(wq.shape, BF16), v(wk.shape, BF16), v(wv.shape, BF16),
            v(wo.shape, BF16), v(cos.shape, F32), v(sin.shape, F32),
            v((half, span, 2 * cols), BF16),
            v((half, block, cols), BF16),
            v((half, length, 2 * cols), BF16),
            v((half, length, cols), BF16),
            v((ntp, seqs, length, cols), BF16),
            v((half, length, cols), BF16),
            v((seqs, heads, length), F32),
            v((half, heads, length), F32),
            v((1, block), F32),
            v((FAR, span // FAR, 2 * HEAD_DIM), BF16),
            v((FAR, rows, HEAD_DIM), BF16),
            v((FAR, rows, HEAD_DIM), BF16),
            v((block, HEAD_DIM), BF16),
            v((GRAN, GRAN), BF16),
            v((grans, GRAN, GRAN + 2 * REACH), F32),
            v((per * rows, per * near_rows), F32),
            v((rows, span // FAR), F32),
            v((FAR, rows, HEAD_DIM), F32),
            v((FAR, rows, HEAD_DIM), F32),
            v((FAR, rows, HEAD_DIM), F32),
            pltpu.SemaphoreType.DMA((seqs + 6,)),
            pltpu.SemaphoreType.DMA((16 * half,)),
            pltpu.SemaphoreType.DMA((16 * half,)),
        ],
        compiler_params=pltpu.CompilerParams(
            collective_id=0, has_side_effects=True, vmem_limit_bytes=56 * 2**20
        ),
        name="layer",
    )(tokens, wq, wk, wv, wo, cos, sin, gain)


def shards(tokens, query_weight, key_weight, value_weight, out_gain, out_weight):
    length = tokens.shape[1]
    sp = lax.axis_index("sp")
    half_dim = HEAD_DIM // 2
    frequency = ROPE_BASE ** (-jnp.arange(half_dim, dtype=F32) / half_dim)
    positions = sp * length + jnp.arange(length, dtype=jnp.int32)
    angles = positions.astype(F32)[:, None] * frequency[None, :]
    cos, sin = jnp.cos(angles), jnp.sin(angles)
    cos = jnp.concatenate([cos, cos], axis=1)
    sin = jnp.concatenate([-sin, sin], axis=1)
    return tuple(
        layer(
            lax.axis_size("sp"), lax.axis_size("tp"), tokens, query_weight, key_weight,
            value_weight, out_weight, cos, sin, out_gain[None, :],
        )
    )


def solution(mesh):
    return jax.shard_map(
        shards,
        mesh=mesh,
        in_specs=(
            P(None, "sp", None),
            P(None, "tp"),
            P(None, "tp"),
            P(None, "tp"),
            P(),
            P(None, "tp"),
        ),
        out_specs=(P(None, "sp", "tp"), P(None, "tp", "sp")),
        check_vma=False,
    )
```

```python
import functools
import math

import jax
import jax.numpy as jnp
from jax import lax
from jax.experimental import pallas as pl
from jax.experimental.pallas import tpu as pltpu
from jax.sharding import PartitionSpec as P

HEAD_DIM = 128
REACH = 64
FAR = 16
NEAR = 4
GRAN = FAR * FAR
ROPE_BASE = 10000.0
MASK_FILL = -1e30
NORM_FLOOR = 1e-06
LOG2E = 1.0 / math.log(2.0)
LN2 = math.log(2.0)
F32 = jnp.float32
BF16 = jnp.bfloat16

MESH = pl.DeviceIdType.MESH


def iota(shape, dim):
    return lax.broadcasted_iota(jnp.int32, shape, dim)


def perm_token(p):
    slot = p // FAR
    a = p % FAR
    residue = slot // NEAR + NEAR * (slot % (FAR // NEAR))
    return a * FAR + residue


def dot_t(a, b):
    return lax.dot_general(a, b, (((1,), (1,)), ((), ())), preferred_element_type=F32)


def layer_kernel(
    nsp, tok_h, wq_h, wk_h, wv_h, wo_h, cos_h, sin_h, gain, out, log_out,
    tok, wq, wk, wv, wo, cos, sin, kn, qn, kvs, qs, gath, outs, logs, lsend, lrow,
    kp, qp, mp, on, perm, bias1, bias4, bias16, o1, m1, l1,
    load_sem, send_sem, recv_sem,
):
    half = tok.shape[0] // 2
    units = kn.shape[0]
    length = tok.shape[1]
    block = 2 * length
    grans = block // GRAN
    wide = REACH * FAR
    side = wide // GRAN
    tail = wide - block
    span = block + 2 * wide
    rows = block // FAR
    key_rows = span // FAR
    near_rows = rows + 2 * FAR
    cols = wq.shape[1]
    heads = cols // HEAD_DIM
    total = nsp * length
    scale = HEAD_DIM**-0.5 * LOG2E
    sp, t = lax.axis_index("sp"), lax.axis_index("tp")
    y, blk = sp % 2, sp // 2
    twin = sp + 1 - 2 * y
    x_peer = (t + 2) % 4
    d_peer = t + 1 - 2 * (t % 2)
    x_d_peer = (d_peer + 2) % 4
    mine, other = y * half, (1 - y) * half

    loads = []

    def load(src, dst):
        copy = pltpu.make_async_copy(src, dst, load_sem.at[len(loads)])
        copy.start()
        loads.append(copy)
        return copy

    got_wk, got_wv = load(wk_h, wk), load(wv_h, wv)
    got_tok = {("m", 0): load(tok_h.at[mine], tok.at[0])}
    got_cos, got_sin = load(cos_h, cos), load(sin_h, sin)
    got_tok["o", 0] = load(tok_h.at[other], tok.at[1])
    for s in range(1, half):
        got_tok["o", s] = load(tok_h.at[other + s], tok.at[2 * s + 1])
        got_tok["m", s] = load(tok_h.at[mine + s], tok.at[2 * s])
    got_wq, got_wo = load(wq_h, wq), load(wo_h, wo)

    barrier = pltpu.get_barrier_semaphore()
    has = {d: (sp + d >= 0) & (sp + d < nsp) for d in (2, -2, 4, -4)}
    reach = {d: has[d] & has[-d] for d in (2, -2)}
    for peer in ((twin, t), (sp, x_peer), (sp, d_peer)):
        pl.semaphore_signal(barrier, inc=1, device_id=peer, device_id_type=MESH)
    count = 3
    for d in (2, -2):
        there = has[d]
        count = count + there.astype(jnp.int32)

        @pl.when(there)
        def _(d=d):
            pl.semaphore_signal(barrier, inc=1, device_id=(sp + d, t), device_id_type=MESH)

    first = pl.multiple_of(y * length, HEAD_DIM)
    second = pl.multiple_of((1 - y) * length, HEAD_DIM)

    def clear(d, at, size):
        @pl.when(jnp.logical_not(has[d]))
        def _():
            for u in range(units):
                kn[u, at : at + size] = jnp.zeros((size, kn.shape[2]), BF16)

    clear(-4, 0, tail)
    clear(-2, tail, block)
    clear(2, wide + block, block)
    clear(4, span - tail, tail)

    numbers = {}

    def copy(name, src, dst, peer):
        n = numbers.setdefault(name, len(numbers))
        return pltpu.make_async_remote_copy(
            src_ref=src, dst_ref=dst, send_sem=send_sem.at[n], recv_sem=recv_sem.at[n],
            device_id=peer, device_id_type=MESH,
        )

    sent = []

    def start(c):
        c.start()
        sent.append((c, None))

    def z_copy(kind, u, d):
        if kind == "T":
            src = wide - tail if d > 0 else wide + block
            dst = 0 if d > 0 else span - tail
            size = tail
        else:
            part = first if kind == "A" else second
            src = wide + part
            dst = (tail if d > 0 else wide + block) + part
            size = length
        return copy(
            (kind, u, d), kn.at[u, pl.ds(src, size)], kn.at[u, pl.ds(dst, size)], (sp + d, t)
        )

    def z_start(kind, u):
        for d in (2, -2):
            c = z_copy(kind, u, d)
            there = reach[d] if kind == "T" else has[d]

            @pl.when(there)
            def _():
                c.start()

            sent.append((c, there))

    def z_wait(kind, u):
        for d in (2, -2):

            @pl.when(has[-2 * d] if kind == "T" else has[-d])
            def _():
                z_copy(kind, u, d).wait_recv()

    def turned(x, w, store):
        a = jnp.dot(x, w[...], preferred_element_type=F32)
        for h in range(heads):
            one = a[:, h * HEAD_DIM : (h + 1) * HEAD_DIM]
            store(h, (one * cos[...] + pltpu.roll(one, HEAD_DIM // 2, 1) * sin[...]).astype(BF16))

    def lanes(n):
        return slice(n * HEAD_DIM, (n + 1) * HEAD_DIM)

    def keys_values(x, put):
        turned(x, wk, lambda h, a: put(2 * h, a))
        v = jnp.dot(x, wv[...], preferred_element_type=F32).astype(BF16)
        for h in range(heads):
            put(2 * h + 1, v[:, lanes(h)])

    def own_kv(s):
        def put(n, a):
            kn[s * heads + n // 2, pl.ds(wide + first, length), lanes(n % 2)] = a

        keys_values(tok[2 * s], put)

    def twin_kv(s):
        def put(n, a):
            kvs[s * heads + n // 2, :, lanes(n % 2)] = a

        keys_values(tok[2 * s + 1], put)

    def own_q(s):
        def put(n, a):
            qn[s * heads + n, pl.ds(first, length)] = a

        turned(tok[2 * s], wq, put)

    def twin_q(s):
        def put(n, a):
            qs[s * heads + n] = a

        turned(tok[2 * s + 1], wq, put)

    def y_kv(u, at):
        return copy(("yk", u), kvs.at[u], kn.at[u, pl.ds(wide + at, length)], (twin, t))

    def y_q(u, at):
        return copy(("yq", u), qs.at[u], qn.at[u, pl.ds(at, length)], (twin, t))

    def of(s):
        return range(s * heads, (s + 1) * heads)

    for c in (got_wk, got_wv, got_cos, got_sin, got_tok["m", 0]):
        c.wait()
    own_kv(0)
    pl.semaphore_wait(barrier, count)
    for u in of(0):
        z_start("A", u)
    got_tok["o", 0].wait()
    twin_kv(0)
    for u in of(0):
        start(y_kv(u, first))
    for s in range(1, half):
        got_tok["o", s].wait()
        got_tok["m", s].wait()
        twin_kv(s)
        for u in of(s):
            start(y_kv(u, first))
        own_kv(s)
    y_kv(0, second).wait_recv()
    z_start("B", 0)
    got_wq.wait()
    twin_q(0)
    own_q(0)
    for u in of(0):
        start(y_q(u, first))
    y_kv(1, second).wait_recv()
    z_start("B", 1)
    for s in range(1, half):
        twin_q(s)
        own_q(s)
        for u in of(s):
            start(y_q(u, first))

    perm[...] = jnp.where(
        iota((GRAN, GRAN), 1) == perm_token(iota((GRAN, GRAN), 0)), 1.0, 0.0
    ).astype(BF16)
    origin = blk * block - wide
    shape = (GRAN, GRAN + 2 * REACH)
    token = perm_token(iota(shape, 0))
    for g in range(grans):
        q_at = wide + g * GRAN + token
        k_at = wide + g * GRAN - REACH + iota(shape, 1)
        ok = (jnp.abs(k_at - q_at) <= REACH) & (k_at + origin >= 0) & (k_at + origin < total)
        bias1[g] = jnp.where(ok, 0.0, MASK_FILL)
    per = FAR // NEAR
    shape = (per * rows, per * near_rows)
    row, col = iota(shape, 0), iota(shape, 1)
    q_at = (row % rows + side * FAR) * FAR + NEAR * (row // rows)
    k_at = (col % near_rows + (side - 1) * FAR) * FAR + NEAR * (col // near_rows)
    ok = (jnp.abs(k_at - q_at) <= REACH * NEAR) & (k_at + origin >= 0) & (k_at + origin < total)
    bias4[...] = jnp.where(ok, 0.0, MASK_FILL)
    shape = (rows, key_rows)
    q_at = iota(shape, 0) + side * FAR
    k_at = iota(shape, 1)
    ok = (
        (jnp.abs(k_at - q_at) <= REACH)
        & (k_at * FAR + origin >= 0)
        & (k_at * FAR + origin < total)
    )
    bias16[...] = jnp.where(ok, 0.0, MASK_FILL)

    def gather_keys(u, slot, chunks):
        for j in chunks:
            moved = jnp.dot(
                perm[...], kn[u, j * GRAN : (j + 1) * GRAN], preferred_element_type=F32
            )
            moved = moved.astype(BF16).reshape(FAR, FAR, 2 * HEAD_DIM)
            kp[slot, :, j * FAR : (j + 1) * FAR] = moved

    ends = tail // GRAN

    def attend_close(u):
        slot = u % 2
        y_q(u, second).wait_recv()
        gather_keys(u, slot, range(ends, span // GRAN - ends))
        for g in range(grans):
            moved = jnp.dot(
                perm[...], qn[u, g * GRAN : (g + 1) * GRAN], preferred_element_type=F32
            )
            moved = moved.astype(BF16)
            qp[slot, :, g * FAR : (g + 1) * FAR] = moved.reshape(FAR, FAR, HEAD_DIM)
            at = wide + g * GRAN - REACH
            k = kn[u, at : at + GRAN + 2 * REACH, :HEAD_DIM]
            v = kn[u, at : at + GRAN + 2 * REACH, HEAD_DIM:]
            sc = dot_t(moved, k) * scale + bias1[g]
            m = jnp.max(sc, axis=1, keepdims=True)
            p = jnp.exp2(sc - m)
            l = jnp.sum(p, axis=1, keepdims=True)
            o = jnp.dot(p.astype(BF16), v, preferred_element_type=F32)
            cut = (FAR, FAR, HEAD_DIM)
            o1[slot, :, g * FAR : (g + 1) * FAR] = o.reshape(cut)
            m1[slot, :, g * FAR : (g + 1) * FAR] = jnp.broadcast_to(m, o.shape).reshape(cut)
            l1[slot, :, g * FAR : (g + 1) * FAR] = jnp.broadcast_to(l, o.shape).reshape(cut)

    def attend_far(u):
        slot = u % 2
        s, h = u // heads, u % heads
        z_wait("T", u)
        gather_keys(u, slot, [*range(ends), *range(span // GRAN - ends, span // GRAN)])
        shuffle = perm[...]
        near_at = (side - 1) * FAR
        for group in range(NEAR):
            sel = slice(group * per, (group + 1) * per)
            flat = (per * rows, HEAD_DIM)
            q = qp[slot, sel].reshape(flat)
            k4 = kp[slot, sel, near_at : near_at + near_rows, :HEAD_DIM].reshape(-1, HEAD_DIM)
            v4 = kp[slot, sel, near_at : near_at + near_rows, HEAD_DIM:].reshape(-1, HEAD_DIM)
            s4 = dot_t(q, k4) * scale + bias4[...]
            b16 = bias16[...]
            s16 = jnp.concatenate(
                [
                    dot_t(qp[slot, group * per + i], kp[slot, group * per + i, :, :HEAD_DIM]) * scale + b16
                    for i in range(per)
                ],
                axis=0,
            )
            m_old = m1[slot, sel].reshape(flat)
            m_row = jnp.maximum(
                jnp.max(s4, axis=1, keepdims=True), jnp.max(s16, axis=1, keepdims=True)
            )
            m_new = jnp.maximum(m_old, m_row)
            m_col = m_new[:, :1]
            keep = jnp.exp2(m_old - m_new)
            p4 = jnp.exp2(s4 - m_col)
            p16 = jnp.exp2(s16 - m_col)
            l = l1[slot, sel].reshape(flat) * keep + (
                jnp.sum(p4, axis=1, keepdims=True) + jnp.sum(p16, axis=1, keepdims=True)
            )
            p16 = p16.astype(BF16)
            o16 = jnp.concatenate(
                [
                    jnp.dot(
                        p16[i * rows : (i + 1) * rows],
                        kp[slot, group * per + i, :, HEAD_DIM:],
                        preferred_element_type=F32,
                    )
                    for i in range(per)
                ],
                axis=0,
            )
            o = o1[slot, sel].reshape(flat) * keep + o16
            o = o + jnp.dot(p4.astype(BF16), v4, preferred_element_type=F32)
            mp[sel] = (o / l).astype(BF16).reshape(per, rows, HEAD_DIM)
            m1[slot, sel] = (m_new * LN2 + jnp.log(l)).reshape(per, rows, HEAD_DIM)
        lane = iota((GRAN, HEAD_DIM), 1)
        for g in range(grans):
            cut = slice(g * FAR, (g + 1) * FAR)
            back = lambda a: lax.dot_general(
                a, shuffle, (((0,), (0,)), ((), ())), preferred_element_type=F32
            )
            merged = lax.dot_general(
                shuffle,
                mp[:, cut].reshape(GRAN, HEAD_DIM),
                (((0,), (0,)), ((), ())),
                preferred_element_type=F32,
            )
            on[g * GRAN : (g + 1) * GRAN] = merged.astype(BF16)
            x = m1[slot, :, cut].reshape(GRAN, HEAD_DIM)
            high = x.astype(BF16).astype(F32)
            mid = (x - high).astype(BF16).astype(F32)
            low = x - high - mid
            terms = jnp.where(
                lane == 0, high, jnp.where(lane == 1, mid, jnp.where(lane == 2, low, 0.0))
            )
            lrow[:, g * GRAN : (g + 1) * GRAN] = jnp.sum(
                back(terms.astype(BF16)), axis=0, keepdims=True
            )
        outs[u] = on[pl.ds(second, length)]
        gath[t, mine + s, h] = on[pl.ds(first, length)]
        logs[mine + s, h] = lrow[:, pl.ds(first, length)]
        lsend[u] = lrow[:, pl.ds(second, length)]
        start(across(u, mine))
        start(piece("xm", u, t, mine, (sp, x_peer)))
        start(piece("dm", u, t, mine, (sp, d_peer)))
        start(log_across(u, mine))

    def across(u, base):
        return copy(
            ("yo", u), outs.at[u], gath.at[t, base + u // heads, u % heads], (twin, t)
        )

    def log_across(u, base):
        return copy(("yl", u), lsend.at[u], logs.at[base + u // heads, u % heads], (twin, t))

    def piece(name, u, owner, base, peer):
        ref = gath.at[owner, base + u // heads, u % heads]
        return copy((name, u), ref, ref, peer)

    def spread(u):
        across(u, other).wait_recv()
        start(piece("xr", u, t, other, (sp, x_peer)))
        start(piece("dr", u, t, other, (sp, d_peer)))
        piece("xm", u, x_peer, mine, (sp, x_peer)).wait_recv()
        start(piece("em", u, x_peer, mine, (sp, d_peer)))

    def spread_twin(u):
        piece("xr", u, x_peer, other, (sp, x_peer)).wait_recv()
        start(piece("er", u, x_peer, other, (sp, d_peer)))
        log_across(u, other).wait_recv()

    def finish(j):
        acc = None
        square = None
        for n in range(gath.shape[0]):
            x = jnp.concatenate([gath[n, j, h] for h in range(heads)], axis=1).astype(F32)
            at = slice(n * cols, (n + 1) * cols)
            scaled = (x * gain[:, at]).astype(BF16)
            term = jnp.dot(scaled, wo[at], preferred_element_type=F32)
            sq = jnp.sum(x * x, axis=1, keepdims=True)
            acc = term if acc is None else acc + term
            square = sq if square is None else square + sq
        out[j] = (acc * lax.rsqrt(square / wo.shape[0] + NORM_FLOOR)).astype(BF16)

    def finish_mine(s):
        for u in of(s):
            piece("dm", u, d_peer, mine, (sp, d_peer)).wait_recv()
            piece("em", u, x_d_peer, mine, (sp, d_peer)).wait_recv()
        finish(mine + s)

    def finish_other(s):
        for u in of(s):
            piece("dr", u, d_peer, other, (sp, d_peer)).wait_recv()
            piece("er", u, x_d_peer, other, (sp, d_peer)).wait_recv()
        finish(other + s)

    def arrived(u):
        z_wait("A", u)
        z_wait("B", u)

    arrived(0)
    z_start("T", 0)
    z_start("A", 2)
    arrived(1)
    z_start("T", 1)
    y_kv(2, second).wait_recv()
    z_start("B", 2)
    z_start("A", 3)
    attend_close(0)
    attend_far(0)
    attend_close(1)
    attend_far(1)
    arrived(2)
    z_start("T", 2)
    y_kv(3, second).wait_recv()
    z_start("B", 3)
    spread(0)
    spread(1)
    attend_close(2)
    spread_twin(0)
    spread_twin(1)
    got_wo.wait()
    arrived(3)
    z_start("T", 3)
    attend_close(3)
    attend_far(2)
    finish_mine(0)
    spread(2)
    attend_far(3)
    spread_twin(2)
    finish_other(0)
    spread(3)
    finish_mine(1)
    spread_twin(3)
    finish_other(1)
    for j in range(logs.shape[0]):
        for h in range(heads):
            log_out[j, h : h + 1] = logs[j, h]
    for c, there in sent:
        if there is None:
            c.wait_send()
        else:

            @pl.when(there)
            def _(c=c):
                c.wait_send()


def layer(nsp, ntp, tokens, wq, wk, wv, wo, cos, sin, gain):
    seqs, length, width = tokens.shape
    half = seqs // 2
    cols = wq.shape[1]
    heads = cols // HEAD_DIM
    block = 2 * length
    wide = REACH * FAR
    span = block + 2 * wide
    rows = block // FAR
    near_rows = rows + 2 * FAR
    per = FAR // NEAR
    grans = block // GRAN
    hbm = pl.BlockSpec(memory_space=pl.ANY)
    vmem = pl.BlockSpec(memory_space=pltpu.VMEM)
    v = pltpu.VMEM
    return pl.pallas_call(
        functools.partial(layer_kernel, nsp),
        in_specs=[hbm] * 7 + [vmem],
        out_specs=[vmem, vmem],
        out_shape=[
            jax.ShapeDtypeStruct((seqs, length, wo.shape[1]), BF16),
            jax.ShapeDtypeStruct((seqs, heads, length), F32),
        ],
        scratch_shapes=[
            v(tokens.shape, BF16), v(wq.shape, BF16), v(wk.shape, BF16), v(wv.shape, BF16),
            v(wo.shape, BF16), v(cos.shape, F32), v(sin.shape, F32),
            v((half * heads, span, 2 * HEAD_DIM), BF16),
            v((half * heads, block, HEAD_DIM), BF16),
            v((half * heads, length, 2 * HEAD_DIM), BF16),
            v((half * heads, length, HEAD_DIM), BF16),
            v((ntp, seqs, heads, length, HEAD_DIM), BF16),
            v((half * heads, length, HEAD_DIM), BF16),
            v((seqs, heads, 1, length), F32),
            v((half * heads, 1, length), F32),
            v((1, block), F32),
            v((2, FAR, span // FAR, 2 * HEAD_DIM), BF16),
            v((2, FAR, rows, HEAD_DIM), BF16),
            v((FAR, rows, HEAD_DIM), BF16),
            v((block, HEAD_DIM), BF16),
            v((GRAN, GRAN), BF16),
            v((grans, GRAN, GRAN + 2 * REACH), F32),
            v((per * rows, per * near_rows), F32),
            v((rows, span // FAR), F32),
            v((2, FAR, rows, HEAD_DIM), F32),
            v((2, FAR, rows, HEAD_DIM), F32),
            v((2, FAR, rows, HEAD_DIM), F32),
            pltpu.SemaphoreType.DMA((seqs + 6,)),
            pltpu.SemaphoreType.DMA((16 * half * heads,)),
            pltpu.SemaphoreType.DMA((16 * half * heads,)),
        ],
        compiler_params=pltpu.CompilerParams(
            collective_id=0, has_side_effects=True, vmem_limit_bytes=56 * 2**20
        ),
        name="layer",
    )(tokens, wq, wk, wv, wo, cos, sin, gain)


def shards(tokens, query_weight, key_weight, value_weight, out_gain, out_weight):
    length = tokens.shape[1]
    sp = lax.axis_index("sp")
    half_dim = HEAD_DIM // 2
    frequency = ROPE_BASE ** (-jnp.arange(half_dim, dtype=F32) / half_dim)
    positions = sp * length + jnp.arange(length, dtype=jnp.int32)
    angles = positions.astype(F32)[:, None] * frequency[None, :]
    cos, sin = jnp.cos(angles), jnp.sin(angles)
    cos = jnp.concatenate([cos, cos], axis=1)
    sin = jnp.concatenate([-sin, sin], axis=1)
    return tuple(
        layer(
            lax.axis_size("sp"), lax.axis_size("tp"), tokens, query_weight, key_weight,
            value_weight, out_weight, cos, sin, out_gain[None, :],
        )
    )


def solution(mesh):
    return jax.shard_map(
        shards,
        mesh=mesh,
        in_specs=(
            P(None, "sp", None),
            P(None, "tp"),
            P(None, "tp"),
            P(None, "tp"),
            P(),
            P(None, "tp"),
        ),
        out_specs=(P(None, "sp", "tp"), P(None, "tp", "sp")),
        check_vma=False,
    )
```

```python
import functools
import math

import jax
import jax.numpy as jnp
import numpy as np
from jax import lax
from jax.experimental import pallas as pl
from jax.experimental.pallas import tpu as pltpu
from jax.sharding import PartitionSpec as P

HEAD_DIM = 128
REACH = 64
FAR = 16
NEAR = 4
GRAN = FAR * FAR
ROPE_BASE = 10000.0
MASK_FILL = -1e30
NORM_FLOOR = 1e-06
LOG2E = 1.0 / math.log(2.0)
LN2 = math.log(2.0)
F32 = jnp.float32
BF16 = jnp.bfloat16

MESH = pl.DeviceIdType.MESH


def iota(shape, dim):
    return lax.broadcasted_iota(jnp.int32, shape, dim)


def perm_token(p):
    slot = p // FAR
    a = p % FAR
    residue = slot // NEAR + NEAR * (slot % (FAR // NEAR))
    return a * FAR + residue


def dot_t(a, b):
    return lax.dot_general(a, b, (((1,), (1,)), ((), ())), preferred_element_type=F32)


def layer_kernel(
    nsp, tok_h, wq_h, wk_h, wv_h, wo_h, cos_h, sin_h, cos_base, sin_base, gain,
    out, log_out,
    tok, wq, wk, wv, wo, cos, sin, kn, qn, kvs, qs, gath, outs, logs, lsend, lrow,
    kp, qp, mp, on, perm, bias1, bias4, bias16, o1, m1, l1,
    load_sem, send_sem, recv_sem,
):
    half = tok.shape[0] // 2
    units = kn.shape[0]
    length = tok.shape[1]
    block = 2 * length
    grans = block // GRAN
    wide = REACH * FAR
    side = wide // GRAN
    tail = wide - block
    span = block + 2 * wide
    rows = block // FAR
    key_rows = span // FAR
    near_rows = rows + 2 * FAR
    cols = wq.shape[1]
    heads = cols // HEAD_DIM
    total = nsp * length
    scale = HEAD_DIM**-0.5 * LOG2E
    sp, t = lax.axis_index("sp"), lax.axis_index("tp")
    y, blk = sp % 2, sp // 2
    twin = sp + 1 - 2 * y
    x_peer = (t + 2) % 4
    d_peer = t + 1 - 2 * (t % 2)
    x_d_peer = (d_peer + 2) % 4
    mine, other = y * half, (1 - y) * half

    loads = []

    def load(src, dst):
        copy = pltpu.make_async_copy(src, dst, load_sem.at[len(loads)])
        copy.start()
        loads.append(copy)
        return copy

    got_cos, got_sin = load(cos_h, cos), load(sin_h, sin)
    got_wk, got_wv = load(wk_h, wk), load(wv_h, wv)
    got_tok = {("m", 0): load(tok_h.at[mine], tok.at[0])}

    barrier = pltpu.get_barrier_semaphore()
    has = {d: (sp + d >= 0) & (sp + d < nsp) for d in (2, -2, 4, -4)}
    reach = {d: has[d] & has[-d] for d in (2, -2)}
    for peer in ((twin, t), (sp, x_peer), (sp, d_peer)):
        pl.semaphore_signal(barrier, inc=1, device_id=peer, device_id_type=MESH)
    count = 3
    for d in (2, -2):
        there = has[d]
        count = count + there.astype(jnp.int32)

        @pl.when(there)
        def _(d=d):
            pl.semaphore_signal(barrier, inc=1, device_id=(sp + d, t), device_id_type=MESH)

    first = pl.multiple_of(y * length, HEAD_DIM)
    second = pl.multiple_of((1 - y) * length, HEAD_DIM)

    def clear(d, at, size):
        @pl.when(jnp.logical_not(has[d]))
        def _():
            for u in range(units):
                kn[u, at : at + size] = jnp.zeros((size, kn.shape[2]), BF16)

    clear(-4, 0, tail)
    clear(-2, tail, block)
    clear(2, wide + block, block)
    clear(4, span - tail, tail)

    numbers = {}

    def copy(name, src, dst, peer):
        n = numbers.setdefault(name, len(numbers))
        return pltpu.make_async_remote_copy(
            src_ref=src, dst_ref=dst, send_sem=send_sem.at[n], recv_sem=recv_sem.at[n],
            device_id=peer, device_id_type=MESH,
        )

    sent = []

    def start(c):
        c.start()
        sent.append((c, None))

    def z_copy(kind, u, d):
        if kind == "T":
            src = wide - tail if d > 0 else wide + block
            dst = 0 if d > 0 else span - tail
            size = tail
        else:
            part = first if kind == "A" else second
            src = wide + part
            dst = (tail if d > 0 else wide + block) + part
            size = length
        return copy(
            (kind, u, d), kn.at[u, pl.ds(src, size)], kn.at[u, pl.ds(dst, size)], (sp + d, t)
        )

    def z_start(kind, u):
        for d in (2, -2):
            c = z_copy(kind, u, d)
            there = reach[d] if kind == "T" else has[d]

            @pl.when(there)
            def _():
                c.start()

            sent.append((c, there))

    def z_wait(kind, u):
        for d in (2, -2):

            @pl.when(has[-2 * d] if kind == "T" else has[-d])
            def _():
                z_copy(kind, u, d).wait_recv()

    def turned(x, w, store):
        a = jnp.dot(x, w[...], preferred_element_type=F32)
        for h in range(heads):
            one = a[:, h * HEAD_DIM : (h + 1) * HEAD_DIM]
            store(h, (one * cos[...] + pltpu.roll(one, HEAD_DIM // 2, 1) * sin[...]).astype(BF16))

    def lanes(n):
        return slice(n * HEAD_DIM, (n + 1) * HEAD_DIM)

    def keys_values(x, put):
        turned(x, wk, lambda h, a: put(2 * h, a))
        v = jnp.dot(x, wv[...], preferred_element_type=F32).astype(BF16)
        for h in range(heads):
            put(2 * h + 1, v[:, lanes(h)])

    def own_kv(s):
        def put(n, a):
            kn[s * heads + n // 2, pl.ds(wide + first, length), lanes(n % 2)] = a

        keys_values(tok[2 * s], put)

    def twin_kv(s):
        def put(n, a):
            kvs[s * heads + n // 2, :, lanes(n % 2)] = a

        keys_values(tok[2 * s + 1], put)

    def own_q(s):
        def put(n, a):
            qn[s * heads + n, pl.ds(first, length)] = a

        turned(tok[2 * s], wq, put)

    def twin_q(s):
        def put(n, a):
            qs[s * heads + n] = a

        turned(tok[2 * s + 1], wq, put)

    def y_kv(u, at):
        return copy(("yk", u), kvs.at[u], kn.at[u, pl.ds(wide + at, length)], (twin, t))

    def y_q(u, at):
        return copy(("yq", u), qs.at[u], qn.at[u, pl.ds(at, length)], (twin, t))

    def of(s):
        return range(s * heads, (s + 1) * heads)

    cos_at, sin_at = cos_base[pl.ds(sp, 1)], sin_base[pl.ds(sp, 1)]
    sign = jnp.where(iota(cos.shape, 1) < HEAD_DIM // 2, -1.0, 1.0)
    got_cos.wait()
    got_sin.wait()
    cos_step, sin_step = cos[...], sin[...]
    cos[...] = cos_step * cos_at - sin_step * sin_at
    sin[...] = (sin_step * cos_at + cos_step * sin_at) * sign
    for c in (got_wk, got_wv, got_tok["m", 0]):
        c.wait()
    got_tok["o", 0] = load(tok_h.at[other], tok.at[1])
    own_kv(0)
    pl.semaphore_wait(barrier, count)
    for u in of(0):
        z_start("A", u)
    got_tok["o", 0].wait()
    got_wq = load(wq_h, wq)
    for s in range(1, half):
        got_tok["o", s] = load(tok_h.at[other + s], tok.at[2 * s + 1])
        got_tok["m", s] = load(tok_h.at[mine + s], tok.at[2 * s])
    got_wo = load(wo_h, wo)
    twin_kv(0)
    for u in of(0):
        start(y_kv(u, first))
    got_wq.wait()
    twin_q(0)
    for u in of(0):
        start(y_q(u, first))
    for s in range(1, half):
        got_tok["o", s].wait()
        got_tok["m", s].wait()
        twin_kv(s)
        for u in of(s):
            start(y_kv(u, first))
        own_kv(s)
    y_kv(0, second).wait_recv()
    z_start("B", 0)
    own_q(0)
    y_kv(1, second).wait_recv()
    z_start("B", 1)
    for s in range(1, half):
        twin_q(s)
        own_q(s)
        for u in of(s):
            start(y_q(u, first))

    perm[...] = jnp.where(
        iota((GRAN, GRAN), 1) == perm_token(iota((GRAN, GRAN), 0)), 1.0, 0.0
    ).astype(BF16)
    origin = blk * block - wide
    shape = (GRAN, GRAN + 2 * REACH)
    token = perm_token(iota(shape, 0))
    for g in range(grans):
        q_at = wide + g * GRAN + token
        k_at = wide + g * GRAN - REACH + iota(shape, 1)
        ok = (jnp.abs(k_at - q_at) <= REACH) & (k_at + origin >= 0) & (k_at + origin < total)
        bias1[g] = jnp.where(ok, 0.0, MASK_FILL)
    per = FAR // NEAR
    shape = (per * rows, per * near_rows)
    row, col = iota(shape, 0), iota(shape, 1)
    q_at = (row % rows + side * FAR) * FAR + NEAR * (row // rows)
    k_at = (col % near_rows + (side - 1) * FAR) * FAR + NEAR * (col // near_rows)
    ok = (jnp.abs(k_at - q_at) <= REACH * NEAR) & (k_at + origin >= 0) & (k_at + origin < total)
    bias4[...] = jnp.where(ok, 0.0, MASK_FILL)
    shape = (rows, key_rows)
    q_at = iota(shape, 0) + side * FAR
    k_at = iota(shape, 1)
    ok = (
        (jnp.abs(k_at - q_at) <= REACH)
        & (k_at * FAR + origin >= 0)
        & (k_at * FAR + origin < total)
    )
    bias16[...] = jnp.where(ok, 0.0, MASK_FILL)

    def gather_keys(u, slot, chunks):
        for j in chunks:
            moved = jnp.dot(
                perm[...], kn[u, j * GRAN : (j + 1) * GRAN], preferred_element_type=F32
            )
            moved = moved.astype(BF16).reshape(FAR, FAR, 2 * HEAD_DIM)
            kp[slot, :, j * FAR : (j + 1) * FAR] = moved

    ends = tail // GRAN

    def attend_close(u):
        slot = u % 2
        y_q(u, second).wait_recv()
        gather_keys(u, slot, range(ends, span // GRAN - ends))
        for g in range(grans):
            moved = jnp.dot(
                perm[...], qn[u, g * GRAN : (g + 1) * GRAN], preferred_element_type=F32
            )
            moved = moved.astype(BF16)
            qp[slot, :, g * FAR : (g + 1) * FAR] = moved.reshape(FAR, FAR, HEAD_DIM)
            at = wide + g * GRAN - REACH
            k = kn[u, at : at + GRAN + 2 * REACH, :HEAD_DIM]
            v = kn[u, at : at + GRAN + 2 * REACH, HEAD_DIM:]
            sc = dot_t(moved, k) * scale + bias1[g]
            m = jnp.max(sc, axis=1, keepdims=True)
            p = jnp.exp2(sc - m)
            l = jnp.sum(p, axis=1, keepdims=True)
            o = jnp.dot(p.astype(BF16), v, preferred_element_type=F32)
            cut = (FAR, FAR, HEAD_DIM)
            o1[slot, :, g * FAR : (g + 1) * FAR] = o.reshape(cut)
            m1[slot, :, g * FAR : (g + 1) * FAR] = jnp.broadcast_to(m, o.shape).reshape(cut)
            l1[slot, :, g * FAR : (g + 1) * FAR] = jnp.broadcast_to(l, o.shape).reshape(cut)

    def attend_far(u):
        slot = u % 2
        s, h = u // heads, u % heads
        z_wait("T", u)
        gather_keys(u, slot, [*range(ends), *range(span // GRAN - ends, span // GRAN)])
        shuffle = perm[...]
        near_at = (side - 1) * FAR
        for group in range(NEAR):
            sel = slice(group * per, (group + 1) * per)
            flat = (per * rows, HEAD_DIM)
            q = qp[slot, sel].reshape(flat)
            k4 = kp[slot, sel, near_at : near_at + near_rows, :HEAD_DIM].reshape(-1, HEAD_DIM)
            v4 = kp[slot, sel, near_at : near_at + near_rows, HEAD_DIM:].reshape(-1, HEAD_DIM)
            s4 = dot_t(q, k4) * scale + bias4[...]
            b16 = bias16[...]
            s16 = jnp.concatenate(
                [
                    dot_t(qp[slot, group * per + i], kp[slot, group * per + i, :, :HEAD_DIM]) * scale + b16
                    for i in range(per)
                ],
                axis=0,
            )
            m_old = m1[slot, sel].reshape(flat)
            m_row = jnp.maximum(
                jnp.max(s4, axis=1, keepdims=True), jnp.max(s16, axis=1, keepdims=True)
            )
            m_new = jnp.maximum(m_old, m_row)
            m_col = m_new[:, :1]
            keep = jnp.exp2(m_old - m_new)
            p4 = jnp.exp2(s4 - m_col)
            p16 = jnp.exp2(s16 - m_col)
            l = l1[slot, sel].reshape(flat) * keep + (
                jnp.sum(p4, axis=1, keepdims=True) + jnp.sum(p16, axis=1, keepdims=True)
            )
            p16 = p16.astype(BF16)
            o16 = jnp.concatenate(
                [
                    jnp.dot(
                        p16[i * rows : (i + 1) * rows],
                        kp[slot, group * per + i, :, HEAD_DIM:],
                        preferred_element_type=F32,
                    )
                    for i in range(per)
                ],
                axis=0,
            )
            o = o1[slot, sel].reshape(flat) * keep + o16
            o = o + jnp.dot(p4.astype(BF16), v4, preferred_element_type=F32)
            mp[sel] = (o / l).astype(BF16).reshape(per, rows, HEAD_DIM)
            m1[slot, sel] = (m_new * LN2 + jnp.log(l)).reshape(per, rows, HEAD_DIM)
        lane = iota((GRAN, HEAD_DIM), 1)
        for g in range(grans):
            cut = slice(g * FAR, (g + 1) * FAR)
            back = lambda a: lax.dot_general(
                a, shuffle, (((0,), (0,)), ((), ())), preferred_element_type=F32
            )
            merged = lax.dot_general(
                shuffle,
                mp[:, cut].reshape(GRAN, HEAD_DIM),
                (((0,), (0,)), ((), ())),
                preferred_element_type=F32,
            )
            on[g * GRAN : (g + 1) * GRAN] = merged.astype(BF16)
            x = m1[slot, :, cut].reshape(GRAN, HEAD_DIM)
            high = x.astype(BF16).astype(F32)
            mid = (x - high).astype(BF16).astype(F32)
            low = x - high - mid
            terms = jnp.where(
                lane == 0, high, jnp.where(lane == 1, mid, jnp.where(lane == 2, low, 0.0))
            )
            lrow[:, g * GRAN : (g + 1) * GRAN] = jnp.sum(
                back(terms.astype(BF16)), axis=0, keepdims=True
            )
        outs[u] = on[pl.ds(second, length)]
        gath[t, mine + s, h] = on[pl.ds(first, length)]
        logs[mine + s, h] = lrow[:, pl.ds(first, length)]
        lsend[u] = lrow[:, pl.ds(second, length)]
        start(across(u, mine))
        start(piece("xm", u, t, mine, (sp, x_peer)))
        start(piece("dm", u, t, mine, (sp, d_peer)))
        start(log_across(u, mine))

    def across(u, base):
        return copy(
            ("yo", u), outs.at[u], gath.at[t, base + u // heads, u % heads], (twin, t)
        )

    def log_across(u, base):
        return copy(("yl", u), lsend.at[u], logs.at[base + u // heads, u % heads], (twin, t))

    def piece(name, u, owner, base, peer):
        ref = gath.at[owner, base + u // heads, u % heads]
        return copy((name, u), ref, ref, peer)

    def spread(u):
        across(u, other).wait_recv()
        start(piece("xr", u, t, other, (sp, x_peer)))
        start(piece("dr", u, t, other, (sp, d_peer)))
        piece("xm", u, x_peer, mine, (sp, x_peer)).wait_recv()
        start(piece("em", u, x_peer, mine, (sp, d_peer)))

    def spread_twin(u):
        piece("xr", u, x_peer, other, (sp, x_peer)).wait_recv()
        start(piece("er", u, x_peer, other, (sp, d_peer)))
        log_across(u, other).wait_recv()

    def finish(j):
        acc = None
        square = None
        for n in range(gath.shape[0]):
            x = jnp.concatenate([gath[n, j, h] for h in range(heads)], axis=1).astype(F32)
            at = slice(n * cols, (n + 1) * cols)
            scaled = (x * gain[:, at]).astype(BF16)
            term = jnp.dot(scaled, wo[at], preferred_element_type=F32)
            sq = jnp.sum(x * x, axis=1, keepdims=True)
            acc = term if acc is None else acc + term
            square = sq if square is None else square + sq
        out[j] = (acc * lax.rsqrt(square / wo.shape[0] + NORM_FLOOR)).astype(BF16)

    def finish_mine(s):
        for u in of(s):
            piece("dm", u, d_peer, mine, (sp, d_peer)).wait_recv()
            piece("em", u, x_d_peer, mine, (sp, d_peer)).wait_recv()
        finish(mine + s)

    def finish_other(s):
        for u in of(s):
            piece("dr", u, d_peer, other, (sp, d_peer)).wait_recv()
            piece("er", u, x_d_peer, other, (sp, d_peer)).wait_recv()
        finish(other + s)

    def arrived(u):
        z_wait("A", u)
        z_wait("B", u)

    arrived(0)
    z_start("T", 0)
    z_start("A", 2)
    arrived(1)
    z_start("T", 1)
    y_kv(2, second).wait_recv()
    z_start("B", 2)
    z_start("A", 3)
    attend_close(0)
    attend_far(0)
    attend_close(1)
    attend_far(1)
    arrived(2)
    z_start("T", 2)
    y_kv(3, second).wait_recv()
    z_start("B", 3)
    spread(0)
    spread(1)
    attend_close(2)
    spread_twin(0)
    spread_twin(1)
    got_wo.wait()
    arrived(3)
    z_start("T", 3)
    attend_close(3)
    attend_far(2)
    finish_mine(0)
    spread(2)
    attend_far(3)
    spread_twin(2)
    finish_other(0)
    spread(3)
    finish_mine(1)
    spread_twin(3)
    finish_other(1)
    for j in range(logs.shape[0]):
        for h in range(heads):
            log_out[j, h : h + 1] = logs[j, h]
    for c, there in sent:
        if there is None:
            c.wait_send()
        else:

            @pl.when(there)
            def _(c=c):
                c.wait_send()


def layer(nsp, ntp, tokens, wq, wk, wv, wo, tables, gain):
    seqs, length, width = tokens.shape
    half = seqs // 2
    cols = wq.shape[1]
    heads = cols // HEAD_DIM
    block = 2 * length
    wide = REACH * FAR
    span = block + 2 * wide
    rows = block // FAR
    near_rows = rows + 2 * FAR
    per = FAR // NEAR
    grans = block // GRAN
    hbm = pl.BlockSpec(memory_space=pl.ANY)
    vmem = pl.BlockSpec(memory_space=pltpu.VMEM)
    v = pltpu.VMEM
    return pl.pallas_call(
        functools.partial(layer_kernel, nsp),
        in_specs=[hbm] * 7 + [vmem] * 3,
        out_specs=[vmem, vmem],
        out_shape=[
            jax.ShapeDtypeStruct((seqs, length, wo.shape[1]), BF16),
            jax.ShapeDtypeStruct((seqs, heads, length), F32),
        ],
        scratch_shapes=[
            v(tokens.shape, BF16), v(wq.shape, BF16), v(wk.shape, BF16), v(wv.shape, BF16),
            v(wo.shape, BF16), v((length, HEAD_DIM), F32), v((length, HEAD_DIM), F32),
            v((half * heads, span, 2 * HEAD_DIM), BF16),
            v((half * heads, block, HEAD_DIM), BF16),
            v((half * heads, length, 2 * HEAD_DIM), BF16),
            v((half * heads, length, HEAD_DIM), BF16),
            v((ntp, seqs, heads, length, HEAD_DIM), BF16),
            v((half * heads, length, HEAD_DIM), BF16),
            v((seqs, heads, 1, length), F32),
            v((half * heads, 1, length), F32),
            v((1, block), F32),
            v((2, FAR, span // FAR, 2 * HEAD_DIM), BF16),
            v((2, FAR, rows, HEAD_DIM), BF16),
            v((FAR, rows, HEAD_DIM), BF16),
            v((block, HEAD_DIM), BF16),
            v((GRAN, GRAN), BF16),
            v((grans, GRAN, GRAN + 2 * REACH), F32),
            v((per * rows, per * near_rows), F32),
            v((rows, span // FAR), F32),
            v((2, FAR, rows, HEAD_DIM), F32),
            v((2, FAR, rows, HEAD_DIM), F32),
            v((2, FAR, rows, HEAD_DIM), F32),
            pltpu.SemaphoreType.DMA((seqs + 6,)),
            pltpu.SemaphoreType.DMA((16 * half * heads,)),
            pltpu.SemaphoreType.DMA((16 * half * heads,)),
        ],
        compiler_params=pltpu.CompilerParams(
            collective_id=0, has_side_effects=True, vmem_limit_bytes=56 * 2**20
        ),
        name="layer",
    )(tokens, wq, wk, wv, wo, *tables, gain)


def shards(tokens, query_weight, key_weight, value_weight, out_gain, out_weight):
    length = tokens.shape[1]
    nsp = lax.axis_size("sp")
    frequency = ROPE_BASE ** (-np.arange(HEAD_DIM // 2) / (HEAD_DIM // 2))
    frequency = np.tile(frequency, 2)[None, :]
    step = np.arange(length)[:, None] * frequency
    base = (np.arange(nsp) * length)[:, None] * frequency
    tables = [
        jnp.asarray(f(a).astype(np.float32)) for a in (step, base) for f in (np.cos, np.sin)
    ]
    return tuple(
        layer(
            nsp, lax.axis_size("tp"), tokens, query_weight, key_weight, value_weight,
            out_weight, tables, out_gain[None, :],
        )
    )


def solution(mesh):
    return jax.shard_map(
        shards,
        mesh=mesh,
        in_specs=(
            P(None, "sp", None),
            P(None, "tp"),
            P(None, "tp"),
            P(None, "tp"),
            P(),
            P(None, "tp"),
        ),
        out_specs=(P(None, "sp", "tp"), P(None, "tp", "sp")),
        check_vma=False,
    )
```
